256 devices in a mesh: kv: 32 (over z, x), tp: 8 (over y, core).
Axes of the slice: x: 4, y: 4, z: 8, core: 2. Of those that a mesh axis runs over, the one named last changes fastest.
Arguments:
- tokens: bfloat16 [256, 4, 4096], P(None, None, 'kv')
- norm_gain: float32 [4096], replicated, may hold values from 0.1 to 1.9
- w_query: bfloat16 [4096, 4096], P('kv', 'tp'), may hold values from -0.09375 to 0.09375
- w_key: bfloat16 [4096, 4096], P('kv', 'tp'), may hold values from -0.09375 to 0.09375
- w_value: bfloat16 [4096, 4096], P('kv', 'tp'), may hold values from -0.09375 to 0.09375
- w_gate: bfloat16 [4096, 4096], P('kv', 'tp'), may hold values from -0.09375 to 0.09375
- w_decay: bfloat16 [4096, 32], replicated, may hold values from -0.09375 to 0.09375
- w_beta: bfloat16 [4096, 32], replicated, may hold values from -0.09375 to 0.09375
- decay_rate: float32 [32], replicated, may hold values from 0.02 to 3
- head_gain: float32 [128], replicated, may hold values from 0.1 to 1.9
- w_out: bfloat16 [4096, 4096], P('tp', 'kv'), may hold values from -0.09375 to 0.09375
- state: float32 [256, 32, 128, 128], P('kv', 'tp'), may hold values from -0.4 to 0.4
- prev_keys: bfloat16 [256, 32, 4, 128], P('kv', 'tp'), may hold values from -6 to 6
- prev_values: bfloat16 [256, 32, 4, 128], P('kv', 'tp'), may hold values from -6 to 6
- prev_log_decay: float32 [256, 32, 4], P('kv', 'tp'), may hold values from -0.7 to -0.02
- prev_beta: float32 [256, 32, 4], P('kv', 'tp'), may hold values from 0.1 to 0.9
- accepted: int32 [256], P('kv'), may hold values from 0 to 4
Outputs:
- mixed: bfloat16 [256, 4, 4096], P('tp', None, 'kv')
- carried: float32 [256, 32, 128, 128], P('kv', 'tp')
The draws below stay inside these ranges and needn't reach their ends.
All inputs are finite; a program needn't handle non-finite values.
Results may differ from the reference program's by a relative error of at most 0.0069.
Values may be sent and summed in bfloat16 or wider, within the bound.
No kernel may reach another device: no remote copies, remote signals or barrier semaphores. Data moves between devices by JAX's collectives and lax.ppermute only.
A program may use at most 128 MiB of HBM per device.

```python
import math
import jax
import jax.numpy as jnp
from jax import lax

D = 4096
HEADS = 32
DK = 128
DV = 128
PROPS = 4
BATCH = 256


def draw_tokens(key, part):
    column = jnp.arange(D, dtype=jnp.float32)
    rising = jnp.exp(math.log(4.0) * column / D)
    values = jax.random.normal(key, (BATCH, PROPS, D), jnp.float32) * rising
    return values.astype(jnp.bfloat16)


def place_ends(result, own_key, least, top_value):
    spot = [jax.random.randint(jax.random.fold_in(own_key, axis), (), 0, length) for axis, length in enumerate(result.shape)]
    widest = result.shape.index(max(result.shape))
    next_to = spot[:widest] + [(spot[widest] + 1) % result.shape[widest]] + spot[widest + 1:]
    return result.at[tuple(spot)].set(least).at[tuple(next_to)].set(top_value)


def block_scale(key, extent, split, low, high):
    def one(dim, parts):
        steps = jax.random.uniform(jax.random.fold_in(jax.random.fold_in(key, 6), dim), (parts,), jnp.float32, low / len(split), high / len(split))
        return jnp.repeat(jnp.exp(steps), extent[dim] // parts).reshape((-1,) + (1,) * (len(extent) - dim - 1))

    factor_of = one(*split[0])
    for cut in split[1:]:
        factor_of = factor_of * one(*cut)
    return factor_of


def scatter_about(key, extent, spread, limit, cuts=(), held_as=jnp.bfloat16):
    drawn = jax.random.normal(key, extent, jnp.float32) * spread
    if len(cuts) > 0:
        drawn = block_scale(key, extent, cuts, -0.22, 0.18) * drawn
    return jnp.clip(drawn, min=-limit, max=limit).astype(held_as)


def setup_inputs(seed: int = 0) -> dict:
    keys = jax.random.split(jax.random.key(seed), 18)
    return {
        "tokens": draw_tokens(jax.random.fold_in(keys[17], 71), 0),
        "norm_gain": jnp.clip(1.0 + 0.18 * jax.random.normal(keys[1], (D,), jnp.float32), 0.1, 1.9),
        "w_query": scatter_about(keys[2], (D, HEADS * DK), D ** -0.5, 0.09375, ((0, 32), (1, 8))),
        "w_key": scatter_about(keys[3], (D, HEADS * DK), D ** -0.5, 0.09375, ((0, 32), (1, 8))),
        "w_value": scatter_about(keys[4], (D, HEADS * DV), D ** -0.5, 0.09375, ((0, 32), (1, 8))),
        "w_gate": scatter_about(keys[5], (D, HEADS * DV), D ** -0.5, 0.09375, ((0, 32), (1, 8))),
        "w_decay": scatter_about(keys[6], (D, HEADS), D ** -0.5, 0.09375),
        "w_beta": scatter_about(keys[7], (D, HEADS), D ** -0.5, 0.09375),
        "decay_rate": jnp.clip(jnp.exp(jax.random.uniform(keys[8], (HEADS,), jnp.float32, math.log(0.02), math.log(3.0))), 0.02, 3.0),
        "head_gain": jnp.clip(1.0 + 0.18 * jax.random.normal(keys[9], (DV,), jnp.float32), 0.1, 1.9),
        "w_out": scatter_about(keys[10], (HEADS * DV, D), (HEADS * DV) ** -0.5, 0.09375, ((0, 8), (1, 32))),
        "state": scatter_about(keys[11], (BATCH, HEADS, DK, DV), 0.05, 0.4, ((0, 32), (1, 8)), jnp.float32),
        "prev_keys": scatter_about(keys[12], (BATCH, HEADS, PROPS, DK), 1.0, 6.0, ((0, 32), (1, 8))),
        "prev_values": scatter_about(keys[13], (BATCH, HEADS, PROPS, DV), 1.0, 6.0, ((0, 32), (1, 8))),
        "prev_log_decay": jnp.clip(-0.7 + 0.68 * jax.random.uniform(keys[14], (BATCH, HEADS, PROPS), jnp.float32) ** block_scale(keys[14], (BATCH, HEADS, PROPS), ((0, 32), (1, 8)), -0.2, 0.2), -0.7, -0.02),
        "prev_beta": jnp.clip(0.1 + 0.79999997 * jax.random.uniform(keys[15], (BATCH, HEADS, PROPS), jnp.float32) ** block_scale(keys[15], (BATCH, HEADS, PROPS), ((0, 32), (1, 8)), -0.2, 0.2), 0.1, 0.9),
        "accepted": place_ends(jax.random.randint(keys[16], (BATCH,), 0, PROPS + 1), jax.random.fold_in(keys[16], 1), 0, PROPS).astype(jnp.int32),
    }


epsilon = 1e-06

def unit_rows(values):
    return values * lax.rsqrt(lax.optimization_barrier(jnp.sum(values * values, axis=-1, keepdims=True)) + epsilon)

def apply_update(matrix, keyvec, valvec, logd, strength):
    decayed = jnp.exp(logd)[..., None, None] * matrix
    predicted = jnp.einsum('bhde,bhd->bhe', decayed, keyvec, precision=lax.Precision.HIGHEST)
    change = strength[..., None] * (valvec - predicted)
    return decayed + jnp.einsum('bhd,bhe->bhde', keyvec, change, precision=lax.Precision.HIGHEST)

def reference(tokens, norm_gain, w_query, w_key, w_value, w_gate, w_decay, w_beta, decay_rate, head_gain, w_out, state, prev_keys, prev_values, prev_log_decay, prev_beta, accepted):
    f32 = jnp.float32
    rowsx = tokens.astype(f32).reshape(BATCH * PROPS, D)
    scale = lax.rsqrt(lax.optimization_barrier(jnp.mean(rowsx * rowsx, axis=1, keepdims=True)) + epsilon)
    normed = (rowsx * scale * norm_gain).astype(jnp.bfloat16)
    qraw = jnp.dot(normed, w_query, preferred_element_type=f32)
    kraw = jnp.dot(normed, w_key, preferred_element_type=f32)
    vraw = jnp.dot(normed, w_value, preferred_element_type=f32)
    zraw = jnp.dot(normed, w_gate, preferred_element_type=f32)
    araw = jnp.dot(normed, w_decay, preferred_element_type=f32)
    braw = jnp.dot(normed, w_beta, preferred_element_type=f32)
    query = unit_rows(jax.nn.silu(qraw).reshape(BATCH, PROPS, HEADS, DK)) * DK ** (-0.5)
    keyrow = unit_rows(jax.nn.silu(kraw).reshape(BATCH, PROPS, HEADS, DK))
    value = jax.nn.silu(vraw).reshape(BATCH, PROPS, HEADS, DV)
    beta = jax.nn.sigmoid(braw).reshape(BATCH, PROPS, HEADS)
    logdecay = (-decay_rate * jax.nn.softplus(araw)).reshape(BATCH, PROPS, HEADS)
    old_keys = unit_rows(prev_keys.astype(f32))
    old_values = prev_values.astype(f32)
    matrix = state
    for proposal in range(PROPS):
        keep = (proposal < accepted).astype(f32)[:, None]
        matrix = apply_update(matrix, old_keys[:, :, proposal], old_values[:, :, proposal], prev_log_decay[:, :, proposal] * keep, prev_beta[:, :, proposal] * keep)
    carried = matrix
    results = []
    for proposal in range(PROPS):
        matrix = apply_update(matrix, keyrow[:, proposal], value[:, proposal], logdecay[:, proposal], beta[:, proposal])
        results.append(jnp.einsum('bhde,bhd->bhe', matrix, query[:, proposal], precision=lax.Precision.HIGHEST))
    attended = jnp.stack(results, axis=1)
    zgate = zraw.reshape(BATCH, PROPS, HEADS, DV)
    headout = attended * lax.rsqrt(lax.optimization_barrier(jnp.mean(attended * attended, axis=-1, keepdims=True)) + epsilon)
    headout = (headout * head_gain * jax.nn.silu(zgate)).astype(jnp.bfloat16).reshape(BATCH * PROPS, HEADS * DV)
    mixed = jnp.dot(headout, w_out, preferred_element_type=f32).astype(jnp.bfloat16)
    return (mixed.reshape(BATCH, PROPS, D), carried)
```

```python
import jax
import jax.numpy as jnp
from jax import lax
from jax.experimental import pallas as pl
from jax.experimental.pallas import tpu as pltpu
from jax.sharding import Mesh
from jax.sharding import PartitionSpec as P

epsilon = 1e-06
ZS, XS, TP = (8, 4, 8)
PROPS = 4
SEQ = 8
HEADS = 4
DK = 128
ROWS = SEQ * PROPS
GROUP = ZS * ROWS
COLS = HEADS * DK
f32 = jnp.float32
bf16 = jnp.bfloat16


VMEM = pl.BlockSpec(memory_space=pltpu.VMEM)
SMEM = pl.BlockSpec(memory_space=pltpu.SMEM)


def ring(step, size):
    return [(i, (i + step) % size) for i in range(size)]


def hidot(a, b):
    return lax.dot_general(
        a, b, (((1,), (0,)), ((), ())), precision=lax.Precision.HIGHEST, preferred_element_type=f32
    )


def spread(rows, matrix_count):
    which = lax.broadcasted_iota(jnp.int32, rows.shape, 0) % matrix_count
    return jnp.concatenate([jnp.where(which == j, rows, 0.0) for j in range(matrix_count)], axis=1)


def lane_sum(a):
    return jnp.sum(a, axis=-1, keepdims=True)


def slab(a, t):
    return a[t * SEQ : (t + 1) * SEQ]


def decays(logs):
    table = {}
    for s in range(-1, PROPS):
        total = None
        for t in range(s + 1, PROPS):
            total = logs[t] if total is None else total + logs[t]
            table[s, t] = jnp.exp(total)
        table[s, s] = None
    return table


def writes(keys, values, strength, decay, read):
    done = []
    for t in range(PROPS):
        predicted = decay[-1, t] * read[t]
        for s in range(t):
            predicted = predicted + (decay[s, t] * lane_sum(keys[s] * keys[t])) * done[s]
        done.append(strength[t] * (values[t] - predicted))
    return done


def carried_kernel(state_ref, keys_ref, values_ref, logs_ref, beta_ref, out_ref):
    lane = lax.broadcasted_iota(jnp.int32, (DK, ROWS), 1) % SEQ
    for h in range(HEADS):
        raw = keys_ref[h]
        unit = raw * lax.rsqrt(lane_sum(raw * raw) + epsilon)
        vals = values_ref[h]
        matrix = state_ref[:, h].reshape(SEQ * DK, DK)
        read = hidot(spread(unit, SEQ), matrix)
        keys = [slab(unit, t) for t in range(PROPS)]
        col = lambda ref, t: ref[:, h * PROPS + t : h * PROPS + t + 1]
        logs = [col(logs_ref, t) for t in range(PROPS)]
        strength = [col(beta_ref, t) for t in range(PROPS)]
        decay = decays(logs)
        done = writes(
            keys, [slab(vals, t) for t in range(PROPS)], strength, decay, [slab(read, t) for t in range(PROPS)]
        )
        last = PROPS - 1
        scaled = [keys[t] if t == last else decay[t, last] * keys[t] for t in range(PROPS)]
        kcols = jnp.concatenate(scaled, axis=0).T
        urows = jnp.concatenate(done, axis=0)
        for j in range(SEQ):
            step = hidot(jnp.where(lane == j, kcols, 0.0), urows)
            keep = decay[-1, last][j : j + 1, :]
            out_ref[j, h] = keep * state_ref[j, h] + step


def first_kernel(x_ref, tok_ref, scale_ref, gain_ref, ab_ref, w0, w1, w2, w3, out_ref, norm_ref):
    x = x_ref[0]
    extra = jnp.zeros((GROUP, 16), f32)
    for r in range(XS):
        at = lax.rem(x + XS - r, XS)
        feats = tok_ref[at].astype(f32)
        piece = (feats * scale_ref[...] * gain_ref[at]).astype(bf16)
        norm_ref[:, r * 128 : (r + 1) * 128] = piece
        extra = extra + lax.dot_general(
            piece, ab_ref[at], (((1,), (1,)), ((), ())), preferred_element_type=f32
        )
    normed = norm_ref[...]
    for half in range(2):
        rows = pl.ds(half * 128, 128)
        weight = jnp.concatenate([w[rows, :] for w in (w0, w1, w2, w3)], axis=0)
        part = jnp.dot(normed, weight, preferred_element_type=f32).astype(bf16)
        out_ref[:, :, half * COLS : (half + 1) * COLS] = part.reshape(ZS, ROWS, COLS)
    high = extra.astype(bf16)
    low = (extra - high.astype(f32)).astype(bf16)
    both = jnp.concatenate([high, low, jnp.zeros((GROUP, 96), bf16)], axis=1)
    out_ref[:, :, 2 * COLS :] = both.reshape(ZS, ROWS, 128)


def second_kernel(norm_ref, w0, w1, w2, w3, out_ref):
    normed = norm_ref[...]
    for half in range(2):
        rows = pl.ds(half * 128, 128)
        weight = jnp.concatenate([w[rows, :] for w in (w0, w1, w2, w3)], axis=0)
        part = jnp.dot(normed, weight, preferred_element_type=f32).astype(bf16)
        out_ref[:, :, half * COLS : (half + 1) * COLS] = part.reshape(ZS, ROWS, COLS)


def unit(a):
    return a * lax.rsqrt(lane_sum(a * a) + epsilon)


def silu(a):
    return a * jax.nn.sigmoid(a)


def attend_kernel(rate_ref, first_ref, second_ref, carried_ref, gain_ref, out_ref):
    def total(ref, lo, hi):
        acc = ref[0, :, lo:hi].astype(f32)
        for s in range(1, ZS):
            acc = acc + ref[s, :, lo:hi].astype(f32)
        return acc

    extra = total(first_ref, 2 * COLS, 2 * COLS + 128)
    for h in range(HEADS):
        lo, hi = (h * DK, (h + 1) * DK)
        query = unit(silu(total(first_ref, lo, hi))) * DK ** (-0.5)
        key = unit(silu(total(first_ref, COLS + lo, COLS + hi)))
        value = silu(total(second_ref, lo, hi))
        gate = silu(total(second_ref, COLS + lo, COLS + hi))
        araw = extra[:, h : h + 1] + extra[:, 16 + h : 17 + h]
        braw = extra[:, 4 + h : 5 + h] + extra[:, 20 + h : 21 + h]
        strength = jax.nn.sigmoid(braw)
        soft = jnp.maximum(araw, 0.0) + jnp.log1p(jnp.exp(-jnp.abs(araw)))
        log = -rate_ref[h] * soft
        matrix = carried_ref[:, h].reshape(SEQ * DK, DK)
        read = hidot(spread(jnp.concatenate([key, query], axis=0), SEQ), matrix)
        keys = [slab(key, t) for t in range(PROPS)]
        decay = decays([slab(log, t) for t in range(PROPS)])
        done = writes(
            keys,
            [slab(value, t) for t in range(PROPS)],
            [slab(strength, t) for t in range(PROPS)],
            decay,
            [slab(read, t) for t in range(PROPS)],
        )
        for t in range(PROPS):
            q = slab(query, t)
            att = decay[-1, t] * slab(read, PROPS + t)
            for s in range(t + 1):
                weight = lane_sum(keys[s] * q)
                if s < t:
                    weight = decay[s, t] * weight
                att = att + weight * done[s]
            att = att * lax.rsqrt(jnp.mean(att * att, axis=-1, keepdims=True) + epsilon)
            head = att * gain_ref[...] * slab(gate, t)
            for s in range(ZS):
                out_ref[s, t * SEQ : (t + 1) * SEQ, lo:hi] = head.astype(bf16)


def project_kernel(x_ref, heads_ref, w0, w1, w2, w3, out_ref):
    x = x_ref[0]
    rows = heads_ref[...].reshape(GROUP, COLS)
    for r, w in enumerate((w0, w1, w2, w3)):
        at = lax.rem(x + XS - r, XS)
        part = jnp.dot(rows, w[...], preferred_element_type=f32).astype(bf16)
        out_ref[pl.ds(at * TP, TP)] = part.reshape(TP, ROWS, 128)


def call(kernel, out, specs, flops, name, scratch=()):
    return pl.pallas_call(
        kernel,
        out_shape=out,
        in_specs=specs,
        out_specs=jax.tree.map(lambda _: VMEM, out),
        scratch_shapes=scratch,
        name=name,
        compiler_params=pltpu.CompilerParams(vmem_limit_bytes=40 * 1024 * 1024),
        cost_estimate=pl.CostEstimate(flops=flops, bytes_accessed=1 << 20, transcendentals=0),
    )


def along_x(shard):
    return lax.ppermute(shard, "x", ring(1, XS)), lax.ppermute(shard, "x", ring(-1, XS))


def per_device(
    tokens,
    norm_gain,
    w_query,
    w_key,
    w_value,
    w_gate,
    w_decay,
    w_beta,
    decay_rate,
    head_gain,
    w_out,
    state,
    prev_keys,
    prev_values,
    prev_log_decay,
    prev_beta,
    accepted,
):
    z = lax.axis_index("z")
    x = lax.axis_index("x")
    tp = lax.axis_index("tp")
    shape = jax.ShapeDtypeStruct
    xs = x.astype(jnp.int32).reshape(1)

    w_qk = jnp.concatenate([w_query, w_key], axis=0)
    w_vz = jnp.concatenate([w_value, w_gate], axis=0)
    qk1, qk3 = along_x(w_qk)
    vz1, vz3 = along_x(w_vz)
    qk2 = lax.ppermute(qk1, "x", ring(1, XS))
    vz2 = lax.ppermute(vz3, "x", ring(-1, XS))

    blocks = tokens.reshape(ZS, XS, SEQ, PROPS, 128)
    blocks = blocks.transpose(1, 0, 3, 2, 4).reshape(XS, GROUP, 128)
    tok = lax.all_to_all(blocks, "x", 0, 0, tiled=True)
    squares = tokens.astype(f32)
    squares = jnp.sum(squares * squares, axis=-1).reshape(ZS, XS, SEQ, PROPS)
    squares = squares.transpose(1, 0, 3, 2).reshape(1, XS, GROUP)
    squares = jnp.broadcast_to(squares, (ZS, XS, GROUP)).reshape(ZS * XS, GROUP)
    squares = jnp.sum(lax.all_to_all(squares, ("z", "x"), 0, 0, tiled=True), axis=0)
    scale = lax.rsqrt(squares / 4096 + epsilon).reshape(GROUP, 1)
    gain = lax.dynamic_slice_in_dim(norm_gain, z * 512, 512, 0).reshape(XS, 1, 128)
    ab = jnp.concatenate(
        [
            lax.dynamic_slice(w.T, (tp * HEADS, z * 512), (HEADS, 512)).reshape(HEADS, XS, 128)
            for w in (w_decay, w_beta)
        ]
        + [jnp.zeros((8, XS, 128), bf16)],
        axis=0,
    ).transpose(1, 0, 2)

    part1, normed = call(
        first_kernel,
        (shape((ZS, ROWS, 2 * COLS + 128), bf16), shape((GROUP, 512), bf16)),
        [SMEM] + [VMEM] * 8,
        2 * GROUP * 512 * 1024,
        "first",
    )(xs, tok, scale, gain, ab, w_qk, qk1, qk2, qk3)
    got1 = lax.all_to_all(part1, "z", 0, 0, tiled=True)
    part2 = call(
        second_kernel,
        shape((ZS, ROWS, 2 * COLS), bf16),
        [VMEM] * 5,
        2 * GROUP * 512 * 1024,
        "second",
    )(normed, w_vz, vz1, vz2, vz3)
    got2 = lax.all_to_all(part2, "z", 0, 0, tiled=True)

    o1, o3 = along_x(w_out)
    o2 = lax.ppermute(o1, "x", ring(1, XS))

    keep = (jnp.arange(PROPS)[None, :] < accepted[:, None]).astype(f32)[:, None, :]
    logs = (prev_log_decay * keep).reshape(SEQ, HEADS * PROPS)
    strengths = (prev_beta * keep).reshape(SEQ, HEADS * PROPS)
    old_keys = prev_keys.astype(f32).transpose(1, 2, 0, 3).reshape(HEADS, ROWS, DK)
    old_values = prev_values.astype(f32).transpose(1, 2, 0, 3).reshape(HEADS, ROWS, DK)
    carried = call(
        carried_kernel, shape(state.shape, f32), [VMEM] * 5, 1 << 31, "carried"
    )(state, old_keys, old_values, logs, strengths)

    rate = lax.dynamic_slice_in_dim(decay_rate, tp * HEADS, HEADS, 0)
    heads = call(
        attend_kernel,
        shape((ZS, ROWS, COLS), bf16),
        [SMEM] + [VMEM] * 4,
        1 << 30,
        "attend",
    )(rate, got1, got2, carried, head_gain.reshape(1, 128))
    heads = lax.all_to_all(heads, "z", 0, 0, tiled=True)
    terms = call(
        project_kernel,
        shape((XS * TP, ROWS, 128), bf16),
        [SMEM] + [VMEM] * 5,
        2 * GROUP * 512 * 512,
        "project",
    )(xs, heads, w_out, o1, o2, o3)
    terms = lax.all_to_all(terms, ("x", "tp"), 0, 0, tiled=True)
    mixed = jnp.sum(terms.reshape(XS, TP, PROPS, SEQ, 128).astype(f32), axis=1)
    mixed = mixed.astype(bf16).transpose(0, 2, 1, 3).reshape(XS * SEQ, PROPS, 128)
    return (mixed, carried)


def solution(mesh):
    grid = Mesh(mesh.devices.reshape(ZS, XS, TP), ("z", "x", "tp"))
    kv = ("z", "x")
    placed = (
        P(None, None, kv),
        P(),
        P(kv, "tp"),
        P(kv, "tp"),
        P(kv, "tp"),
        P(kv, "tp"),
        P(),
        P(),
        P(),
        P(),
        P("tp", kv),
        P(kv, "tp", None, None),
        P(kv, "tp", None, None),
        P(kv, "tp", None, None),
        P(kv, "tp", None),
        P(kv, "tp", None),
        P(kv),
    )
    return jax.shard_map(
        per_device,
        mesh=grid,
        in_specs=placed,
        out_specs=(P("tp", None, kv), P(kv, "tp", None, None)),
        check_vma=False,
    )
```

```python
import jax
import jax.numpy as jnp
from jax import lax
from jax.experimental import pallas as pl
from jax.experimental.pallas import tpu as pltpu
from jax.sharding import Mesh
from jax.sharding import PartitionSpec as P

epsilon = 1e-06
ZS, XS, TP = (8, 4, 8)
PROPS = 4
SEQ = 8
HEADS = 4
DK = 128
ROWS = SEQ * PROPS
GROUP = ZS * ROWS
COLS = HEADS * DK
WIDE = 4 * COLS + 128
FOLD = ZS // 2 + 1
f32 = jnp.float32
bf16 = jnp.bfloat16


VMEM = pl.BlockSpec(memory_space=pltpu.VMEM)
ANY = pl.BlockSpec(memory_space=pl.ANY)
SMEM = pl.BlockSpec(memory_space=pltpu.SMEM)


def ring(step, size):
    return [(i, (i + step) % size) for i in range(size)]


def hidot(a, b):
    return lax.dot_general(
        a, b, (((1,), (0,)), ((), ())), precision=lax.Precision.HIGHEST, preferred_element_type=f32
    )


def spread(rows, matrix_count):
    which = lax.broadcasted_iota(jnp.int32, rows.shape, 0) % matrix_count
    return jnp.concatenate([jnp.where(which == j, rows, 0.0) for j in range(matrix_count)], axis=1)


def lane_sum(a):
    return jnp.sum(a, axis=-1, keepdims=True)


def slab(a, t):
    return a[t * SEQ : (t + 1) * SEQ]


def decays(logs):
    table = {}
    for s in range(-1, PROPS):
        total = None
        for t in range(s + 1, PROPS):
            total = logs[t] if total is None else total + logs[t]
            table[s, t] = jnp.exp(total)
        table[s, s] = None
    return table


def writes(keys, values, strength, decay, read):
    done = []
    for t in range(PROPS):
        predicted = decay[-1, t] * read[t]
        for s in range(t):
            predicted = predicted + (decay[s, t] * lane_sum(keys[s] * keys[t])) * done[s]
        done.append(strength[t] * (values[t] - predicted))
    return done


def head_copies(outer, inner, sems, inward):
    pairs = [(outer.at[:, h], inner.at[h]) for h in range(HEADS)]
    return [
        pltpu.make_async_copy(*(pair if inward else pair[::-1]), sems.at[h]) for h, pair in enumerate(pairs)
    ]


def carried_kernel(state_ref, keys_ref, values_ref, logs_ref, beta_ref, out_ref, old_ref, new_ref, sems):
    loads = head_copies(state_ref, old_ref, sems.at[0], True)
    stores = head_copies(out_ref, new_ref, sems.at[1], False)
    for load in loads:
        load.start()
    lane = lax.broadcasted_iota(jnp.int32, (DK, ROWS), 1) % SEQ
    for h in range(HEADS):
        raw = keys_ref[h]
        unit = raw * lax.rsqrt(lane_sum(raw * raw) + epsilon)
        vals = values_ref[h]
        loads[h].wait()
        matrix = old_ref[h].reshape(SEQ * DK, DK)
        read = hidot(spread(unit, SEQ), matrix)
        keys = [slab(unit, t) for t in range(PROPS)]
        col = lambda ref, t: ref[:, h * PROPS + t : h * PROPS + t + 1]
        logs = [col(logs_ref, t) for t in range(PROPS)]
        strength = [col(beta_ref, t) for t in range(PROPS)]
        decay = decays(logs)
        done = writes(
            keys, [slab(vals, t) for t in range(PROPS)], strength, decay, [slab(read, t) for t in range(PROPS)]
        )
        last = PROPS - 1
        scaled = [keys[t] if t == last else decay[t, last] * keys[t] for t in range(PROPS)]
        kcols = jnp.concatenate(scaled, axis=0).T
        urows = jnp.concatenate(done, axis=0)
        for j in range(SEQ):
            step = hidot(jnp.where(lane == j, kcols, 0.0), urows)
            keep = decay[-1, last][j : j + 1, :]
            new_ref[h, j] = keep * old_ref[h, j] + step
        stores[h].start()
    for store in stores:
        store.wait()


def squares_kernel(tok_ref, out_ref):
    total = jnp.zeros((GROUP, 128), f32)
    for s in range(XS):
        feats = tok_ref[s].astype(f32)
        total = total + feats * feats
    ones = jnp.ones((8, 128), f32)
    rows = lax.dot_general(
        ones, total, (((1,), (1,)), ((), ())), precision=lax.Precision.HIGHEST, preferred_element_type=f32
    )
    for s in range(ZS):
        out_ref[s] = rows[0:1]


def columns_kernel(place_ref, tok_ref, squares_ref, gain_ref, ab_ref, *refs):
    pieces, (own_ref, *block_refs, norm_ref, scale_ref) = (refs[: 2 * XS], refs[2 * XS :])
    z, x = (place_ref[0], place_ref[1])
    squares = squares_ref[0]
    for s in range(1, ZS):
        squares = squares + squares_ref[s]
    scale = lax.rsqrt(squares / 4096 + epsilon)
    scale_ref[...] = jnp.broadcast_to(scale, (128, GROUP)).T
    extra = jnp.zeros((GROUP, 16), f32)
    for r in range(XS):
        at = lax.rem(x + XS - r, XS)
        for d in range(ZS):
            rows = pl.ds(pl.multiple_of(lax.rem(z + d, ZS) * ROWS, ROWS), ROWS)
            feats = tok_ref[at, rows, :].astype(f32)
            piece = (feats * scale_ref[rows, :] * gain_ref[at]).astype(bf16)
            norm_ref[d * ROWS : (d + 1) * ROWS, r * 128 : (r + 1) * 128] = piece
        extra = extra + lax.dot_general(
            norm_ref[:, r * 128 : (r + 1) * 128],
            ab_ref[at],
            (((1,), (1,)), ((), ())),
            preferred_element_type=f32,
        )
    normed = norm_ref[...]

    def put(lo, hi, part):
        for d in range(ZS):
            rows = part[d * ROWS : (d + 1) * ROWS]
            if d == 0:
                own_ref[:, lo:hi] = rows
            else:
                ref = block_refs[d - 1]
                ref[:, lo:hi] = rows.astype(ref.dtype)

    for pair in range(2):
        mine = pieces[pair * XS : (pair + 1) * XS]
        for half in range(2):
            weight = jnp.concatenate([w[half * 128 : (half + 1) * 128, :] for w in mine], axis=0)
            at = (2 * pair + half) * COLS
            put(at, at + COLS, jnp.dot(normed, weight, preferred_element_type=f32))
    zero = jnp.zeros((GROUP, 112), f32)
    put(4 * COLS, WIDE, jnp.concatenate([extra, zero], axis=1))
    low = extra - extra.astype(bf16).astype(f32)
    for d in range(1, ZS):
        if d != FOLD:
            rows = low[d * ROWS : (d + 1) * ROWS]
            block_refs[d - 1][:, 4 * COLS + 16 : 4 * COLS + 32] = rows.astype(bf16)


def fold_kernel(came_ref, own_ref, out_ref):
    total = came_ref[...].astype(f32) + own_ref[...]
    out_ref[...] = total.astype(bf16)
    at = 4 * COLS
    extra = total[:, at : at + 16] + total[:, at + 16 : at + 32]
    high = extra.astype(bf16)
    out_ref[:, at : at + 16] = high
    out_ref[:, at + 16 : at + 32] = (extra - high.astype(f32)).astype(bf16)


def unit(a):
    return a * lax.rsqrt(lane_sum(a * a) + epsilon)


def silu(a):
    return a * jax.nn.sigmoid(a)


def attend_kernel(rate_ref, carried_ref, gain_ref, own_ref, *refs):
    came, (out_ref, rows_ref, heads_ref) = (refs[:-3], refs[-3:])

    def total(lo, hi):
        acc = own_ref[:, lo:hi]
        for ref in came:
            acc = acc + ref[:, lo:hi].astype(f32)
        return acc

    def regroup(index, rows):
        rows_ref[index] = rows
        return jnp.concatenate(
            [rows_ref[index, pl.ds(t, SEQ, stride=PROPS), :] for t in range(PROPS)], axis=0
        )

    extra = regroup(0, total(4 * COLS, WIDE))
    for h in range(HEADS):
        lo, hi = (h * DK, (h + 1) * DK)
        spot = 1 + 4 * h
        query = unit(silu(regroup(spot, total(lo, hi)))) * DK ** (-0.5)
        key = unit(silu(regroup(spot + 1, total(COLS + lo, COLS + hi))))
        value = silu(regroup(spot + 2, total(2 * COLS + lo, 2 * COLS + hi)))
        gate = silu(regroup(spot + 3, total(3 * COLS + lo, 3 * COLS + hi)))
        araw = extra[:, h : h + 1] + extra[:, 16 + h : 17 + h]
        braw = extra[:, 4 + h : 5 + h] + extra[:, 20 + h : 21 + h]
        strength = jax.nn.sigmoid(braw)
        soft = jnp.maximum(araw, 0.0) + jnp.log1p(jnp.exp(-jnp.abs(araw)))
        log = -rate_ref[h] * soft
        matrix = carried_ref[:, h].reshape(SEQ * DK, DK)
        read = hidot(spread(jnp.concatenate([key, query], axis=0), SEQ), matrix)
        keys = [slab(key, t) for t in range(PROPS)]
        decay = decays([slab(log, t) for t in range(PROPS)])
        done = writes(
            keys,
            [slab(value, t) for t in range(PROPS)],
            [slab(strength, t) for t in range(PROPS)],
            decay,
            [slab(read, t) for t in range(PROPS)],
        )
        for t in range(PROPS):
            q = slab(query, t)
            att = decay[-1, t] * slab(read, PROPS + t)
            for s in range(t + 1):
                weight = lane_sum(keys[s] * q)
                if s < t:
                    weight = decay[s, t] * weight
                att = att + weight * done[s]
            att = att * lax.rsqrt(jnp.mean(att * att, axis=-1, keepdims=True) + epsilon)
            heads_ref[h, pl.ds(t, SEQ, stride=PROPS), :] = att * gain_ref[...] * slab(gate, t)
        head = heads_ref[h].astype(bf16)
        for s in range(ZS):
            out_ref[s, :, lo:hi] = head


def project_kernel(x_ref, heads_ref, w0, w1, w2, w3, out_ref):
    x = x_ref[0]
    rows = heads_ref[...].reshape(GROUP, COLS)
    for r, w in enumerate((w0, w1, w2, w3)):
        at = lax.rem(x + XS - r, XS)
        part = jnp.dot(rows, w[...], preferred_element_type=f32).astype(bf16)
        out_ref[pl.ds(at * TP, TP)] = part.reshape(TP, ROWS, 128)


def final_kernel(terms_ref, out_ref):
    for s in range(XS):
        total = terms_ref[s * TP].astype(f32)
        for t in range(1, TP):
            total = total + terms_ref[s * TP + t].astype(f32)
        out_ref[pl.ds(s * ROWS, ROWS), :] = total.astype(bf16)


def call(kernel, out, specs, flops, scratch=(), grant=16384, placed=VMEM):
    return pl.pallas_call(
        kernel,
        out_shape=out,
        in_specs=specs,
        out_specs=jax.tree.map(lambda _: placed, out),
        scratch_shapes=scratch,
        compiler_params=pltpu.CompilerParams(vmem_limit_bytes=grant * 1024),
        cost_estimate=pl.CostEstimate(flops=flops, bytes_accessed=1 << 20, transcendentals=0),
    )


def shift(shard, step, axis="x"):
    return lax.ppermute(shard, axis, ring(step, lax.axis_size(axis)))


def exchange(blocks, axes):
    return lax.all_to_all(blocks, axes, 0, 0, tiled=True)


def step(
    tokens,
    norm_gain,
    w_query,
    w_key,
    w_value,
    w_gate,
    w_decay,
    w_beta,
    decay_rate,
    head_gain,
    w_out,
    state,
    prev_keys,
    prev_values,
    prev_log_decay,
    prev_beta,
    accepted,
):
    z = lax.axis_index("z")
    x = lax.axis_index("x")
    tp = lax.axis_index("tp")
    shape = jax.ShapeDtypeStruct
    xs = x.astype(jnp.int32).reshape(1)

    blocks = tokens.reshape(ZS, XS, ROWS, 128).transpose(1, 0, 2, 3).reshape(XS, GROUP, 128)
    tok = exchange(blocks, "x")

    w_qk = jnp.concatenate([w_query, w_key], axis=0)
    w_vz = jnp.concatenate([w_value, w_gate], axis=0)
    qk1 = shift(w_qk, 1)
    vz3 = shift(w_vz, -1)
    vz1 = shift(w_vz, 1)
    qk3 = shift(w_qk, -1)
    qk2 = shift(qk1, 1)
    vz2 = shift(vz3, -1)

    squares = call(squares_kernel, shape((ZS, 1, GROUP), f32), [VMEM], 1 << 20)(tok)
    squares = exchange(squares, "z")
    gain = lax.dynamic_slice_in_dim(norm_gain, z * 512, 512, 0).reshape(XS, 1, 128)
    ab = jnp.concatenate(
        [
            lax.dynamic_slice(w.T, (tp * HEADS, z * 512), (HEADS, 512)).reshape(HEADS, XS, 128)
            for w in (w_decay, w_beta)
        ]
        + [jnp.zeros((8, XS, 128), bf16)],
        axis=0,
    ).transpose(1, 0, 2)

    types = [f32 if d in (0, FOLD) else bf16 for d in range(ZS)]
    own, *block = call(
        columns_kernel,
        [shape((ROWS, WIDE), t) for t in types],
        [SMEM] + [VMEM] * 12,
        2 * GROUP * 512 * 2048,
        [pltpu.VMEM((GROUP, 512), bf16), pltpu.VMEM((GROUP, 128), f32)],
    )(jnp.stack([z, x]).astype(jnp.int32), tok, squares, gain, ab, w_qk, qk1, qk2, qk3, w_vz, vz1, vz2, vz3)
    came = {4: shift(block[3], -1, "z")}
    for d in (3, 2, 6, 1, 7):
        came[d] = shift(block[d - 1], d, "z")
    folded = call(fold_kernel, shape((ROWS, WIDE), bf16), [VMEM] * 2, 1 << 20)(came.pop(4), block[4])
    came[5] = shift(folded, 5, "z")

    o1 = shift(w_out, 1)
    o3 = shift(w_out, -1)
    o2 = shift(o1, 1)

    keep = (jnp.arange(PROPS)[None, :] < accepted[:, None]).astype(f32)[:, None, :]
    logs = (prev_log_decay * keep).reshape(SEQ, HEADS * PROPS)
    strengths = (prev_beta * keep).reshape(SEQ, HEADS * PROPS)
    old_keys = prev_keys.astype(f32).transpose(1, 2, 0, 3).reshape(HEADS, ROWS, DK)
    old_values = prev_values.astype(f32).transpose(1, 2, 0, 3).reshape(HEADS, ROWS, DK)
    whole = shape(state.shape, f32)
    buffer = pltpu.VMEM((HEADS, SEQ, DK, DK), f32)
    carried = call(
        carried_kernel,
        whole,
        [ANY] + [VMEM] * 4,
        1 << 31,
        [buffer, buffer, pltpu.SemaphoreType.DMA((2, HEADS))],
        60 * 1024,
        ANY,
    )(state, old_keys, old_values, logs, strengths)

    rate = lax.dynamic_slice_in_dim(decay_rate, tp * HEADS, HEADS, 0)
    heads = call(
        attend_kernel,
        shape((ZS, ROWS, COLS), bf16),
        [SMEM] + [VMEM] * 9,
        1 << 30,
        [
            pltpu.VMEM((1 + 4 * HEADS, ROWS, DK), f32),
            pltpu.VMEM((HEADS, ROWS, DK), f32),
        ],
    )(rate, carried, head_gain.reshape(1, 128), own, *came.values())
    heads = exchange(heads, "z")
    terms = call(
        project_kernel,
        shape((XS * TP, ROWS, 128), bf16),
        [SMEM] + [VMEM] * 5,
        2 * GROUP * 512 * 512,
    )(xs, heads, w_out, o1, o2, o3)
    terms = exchange(terms, ("x", "tp"))
    mixed = call(final_kernel, shape((XS * ROWS, 128), bf16), [VMEM], 1 << 20)(terms)
    return (mixed.reshape(XS * SEQ, PROPS, 128), carried)


def solution(mesh):
    grid = Mesh(mesh.devices.reshape(ZS, XS, TP), ("z", "x", "tp"))
    kv = ("z", "x")
    placed = (
        P(None, None, kv),
        P(),
        P(kv, "tp"),
        P(kv, "tp"),
        P(kv, "tp"),
        P(kv, "tp"),
        P(),
        P(),
        P(),
        P(),
        P("tp", kv),
        P(kv, "tp", None, None),
        P(kv, "tp", None, None),
        P(kv, "tp", None, None),
        P(kv, "tp", None),
        P(kv, "tp", None),
        P(kv),
    )
    return jax.shard_map(
        step,
        mesh=grid,
        in_specs=placed,
        out_specs=(P("tp", None, kv), P(kv, "tp", None, None)),
        check_vma=False,
    )
```

```python
import jax
import jax.numpy as jnp
from jax import lax
from jax.experimental import pallas as pl
from jax.experimental.pallas import tpu as pltpu
from jax.sharding import Mesh
from jax.sharding import PartitionSpec as P

epsilon = 1e-06
ZS, XS, TP = (8, 4, 8)
PROPS = 4
SEQ = 8
HEADS = 4
DK = 128
ROWS = SEQ * PROPS
GROUP = ZS * ROWS
COLS = HEADS * DK
WIDE = 4 * COLS + 128
FOLD = ZS // 2 + 1
f32 = jnp.float32
bf16 = jnp.bfloat16


VMEM = pl.BlockSpec(memory_space=pltpu.VMEM)
ANY = pl.BlockSpec(memory_space=pl.ANY)
SMEM = pl.BlockSpec(memory_space=pltpu.SMEM)


def ring(step, size):
    return [(i, (i + step) % size) for i in range(size)]


def hidot(a, b):
    return lax.dot_general(
        a, b, (((1,), (0,)), ((), ())), precision=lax.Precision.HIGHEST, preferred_element_type=f32
    )


def spread(rows, matrix_count):
    which = lax.broadcasted_iota(jnp.int32, rows.shape, 0) % matrix_count
    return jnp.concatenate([jnp.where(which == j, rows, 0.0) for j in range(matrix_count)], axis=1)


def lane_sum(a):
    return jnp.sum(a, axis=-1, keepdims=True)


def slab(a, t):
    return a[t * SEQ : (t + 1) * SEQ]


def decays(logs):
    table = {}
    for s in range(-1, PROPS):
        total = None
        for t in range(s + 1, PROPS):
            total = logs[t] if total is None else total + logs[t]
            table[s, t] = jnp.exp(total)
        table[s, s] = None
    return table


def writes(keys, values, strength, decay, read):
    done = []
    for t in range(PROPS):
        predicted = decay[-1, t] * read[t]
        for s in range(t):
            predicted = predicted + (decay[s, t] * lane_sum(keys[s] * keys[t])) * done[s]
        done.append(strength[t] * (values[t] - predicted))
    return done


def head_copies(outer, inner, sems, inward):
    pairs = [(outer.at[:, h], inner.at[h]) for h in range(HEADS)]
    return [
        pltpu.make_async_copy(*(pair if inward else pair[::-1]), sems.at[h]) for h, pair in enumerate(pairs)
    ]


def carried_kernel(state_ref, keys_ref, values_ref, logs_ref, beta_ref, out_ref, near_ref, old_ref, new_ref, sems):
    loads = head_copies(state_ref, old_ref, sems.at[0], True)
    stores = head_copies(out_ref, new_ref, sems.at[1], False)
    for load in loads:
        load.start()
    lane = lax.broadcasted_iota(jnp.int32, (DK, ROWS), 1) % SEQ
    for h in range(HEADS):
        raw = keys_ref[h]
        unit = raw * lax.rsqrt(lane_sum(raw * raw) + epsilon)
        vals = values_ref[h]
        loads[h].wait()
        matrix = old_ref[h].reshape(SEQ * DK, DK)
        read = hidot(spread(unit, SEQ), matrix)
        keys = [slab(unit, t) for t in range(PROPS)]
        col = lambda ref, t: ref[:, h * PROPS + t : h * PROPS + t + 1]
        logs = [col(logs_ref, t) for t in range(PROPS)]
        strength = [col(beta_ref, t) for t in range(PROPS)]
        decay = decays(logs)
        done = writes(
            keys, [slab(vals, t) for t in range(PROPS)], strength, decay, [slab(read, t) for t in range(PROPS)]
        )
        last = PROPS - 1
        scaled = [keys[t] if t == last else decay[t, last] * keys[t] for t in range(PROPS)]
        kcols = jnp.concatenate(scaled, axis=0).T
        urows = jnp.concatenate(done, axis=0)
        for j in range(SEQ):
            step = hidot(jnp.where(lane == j, kcols, 0.0), urows)
            keep = decay[-1, last][j : j + 1, :]
            fresh = keep * old_ref[h, j] + step
            new_ref[h, j] = fresh
            near_ref[h, j] = fresh
        stores[h].start()
    for store in stores:
        store.wait()


def blocks_kernel(tok_ref, out_ref):
    for s in range(XS):
        for d in range(ZS):
            out_ref[s, d * ROWS : (d + 1) * ROWS, :] = tok_ref[d, s]


def columns_kernel(z_ref, x_ref, tp_ref, tok_ref, gain_ref, decay_ref, beta_ref, *refs):
    pieces, (own_ref, *block_refs, high_ref, low_ref) = (refs[: 2 * XS], refs[2 * XS :])
    z, x, tp = (z_ref[0], x_ref[0], tp_ref[0])
    every = jnp.zeros((GROUP, 2 * HEADS * TP), f32)
    squares = jnp.zeros((GROUP, 128), f32)
    for r in range(XS):
        at = lax.rem(x + XS - r, XS)
        gain = gain_ref[pl.ds(z * XS + at, 1), :]
        feats = jnp.concatenate(
            [
                tok_ref[at, pl.ds(pl.multiple_of(lax.rem(z + d, ZS) * ROWS, ROWS), ROWS), :]
                for d in range(ZS)
            ],
            axis=0,
        ).astype(f32)
        squares = squares + feats * feats
        feats = feats * gain
        high = feats.astype(bf16)
        low = (feats - high.astype(f32)).astype(bf16)
        high_ref[:, r * 128 : (r + 1) * 128] = high
        low_ref[:, r * 128 : (r + 1) * 128] = low
        lanes = pl.ds(pl.multiple_of((z * XS + at) * 128, 128), 128)
        small = jnp.concatenate([decay_ref[:, lanes], beta_ref[:, lanes]], axis=0)
        for part in (high, low):
            every = every + lax.dot_general(
                part, small, (((1,), (1,)), ((), ())), preferred_element_type=f32
            )
    row = lax.broadcasted_iota(jnp.int32, (2 * HEADS * TP, 16), 0)
    col = lax.broadcasted_iota(jnp.int32, (2 * HEADS * TP, 16), 1)
    wanted = jnp.where(col < HEADS, col, col - HEADS + HEADS * TP) + tp * HEADS
    pick = jnp.logical_and(row == wanted, col < 2 * HEADS)
    extra = hidot(every, jnp.where(pick, 1.0, 0.0))
    col = lax.broadcasted_iota(jnp.int32, (GROUP, 16), 1)
    extra = jnp.where(col == 2 * HEADS, lane_sum(squares), extra)
    high = high_ref[...]
    low = low_ref[...]

    def put(lo, hi, part):
        for d in range(ZS):
            rows = part[d * ROWS : (d + 1) * ROWS]
            if d == 0:
                own_ref[:, lo:hi] = rows
            else:
                ref = block_refs[d - 1]
                ref[:, lo:hi] = rows.astype(ref.dtype)

    for pair in range(2):
        mine = pieces[pair * XS : (pair + 1) * XS]
        for half in range(2):
            weight = jnp.concatenate([w[:, half * COLS : (half + 1) * COLS] for w in mine], axis=0)
            at = (2 * pair + half) * COLS
            total = jnp.dot(high, weight, preferred_element_type=f32)
            total = total + jnp.dot(low, weight, preferred_element_type=f32)
            put(at, at + COLS, total)
    zero = jnp.zeros((GROUP, 112), f32)
    put(4 * COLS, WIDE, jnp.concatenate([extra, zero], axis=1))
    rest = extra - extra.astype(bf16).astype(f32)
    for d in range(1, ZS):
        if d != FOLD:
            rows = rest[d * ROWS : (d + 1) * ROWS]
            block_refs[d - 1][:, 4 * COLS + 16 : 4 * COLS + 32] = rows.astype(bf16)


def fold_kernel(came_ref, own_ref, out_ref):
    total = came_ref[...].astype(f32) + own_ref[...]
    out_ref[...] = total.astype(bf16)
    at = 4 * COLS
    extra = total[:, at : at + 16] + total[:, at + 16 : at + 32]
    high = extra.astype(bf16)
    out_ref[:, at : at + 16] = high
    out_ref[:, at + 16 : at + 32] = (extra - high.astype(f32)).astype(bf16)


def unit(a):
    return a * lax.rsqrt(lane_sum(a * a) + epsilon)


def silu(a):
    return a * jax.nn.sigmoid(a)


def attend_kernel(tp_ref, rate_ref, carried_ref, gain_ref, own_ref, *refs):
    came, (out_ref, rows_ref, heads_ref) = (refs[:-3], refs[-3:])

    def total(lo, hi):
        acc = own_ref[:, lo:hi]
        for ref in came:
            acc = acc + ref[:, lo:hi].astype(f32)
        return acc

    def regroup(index, rows):
        rows_ref[index] = rows
        return jnp.concatenate(
            [rows_ref[index, pl.ds(t, SEQ, stride=PROPS), :] for t in range(PROPS)], axis=0
        )

    extra = regroup(0, total(4 * COLS, WIDE))
    extra = extra[:, :16] + extra[:, 16:32]
    scale = lax.rsqrt(extra[:, 2 * HEADS : 2 * HEADS + 1] / 4096 + epsilon)

    def raw(index, lo, hi):
        return regroup(index, total(lo, hi)) * scale

    for h in range(HEADS):
        lo, hi = (h * DK, (h + 1) * DK)
        spot = 1 + 4 * h
        query = unit(silu(raw(spot, lo, hi))) * DK ** (-0.5)
        key = unit(silu(raw(spot + 1, COLS + lo, COLS + hi)))
        value = silu(raw(spot + 2, 2 * COLS + lo, 2 * COLS + hi))
        gate = silu(raw(spot + 3, 3 * COLS + lo, 3 * COLS + hi))
        araw = extra[:, h : h + 1] * scale
        braw = extra[:, HEADS + h : HEADS + h + 1] * scale
        strength = jax.nn.sigmoid(braw)
        soft = jnp.maximum(araw, 0.0) + jnp.log1p(jnp.exp(-jnp.abs(araw)))
        mine = lax.broadcasted_iota(jnp.int32, rate_ref.shape, 1) == tp_ref[0] * HEADS + h
        log = -lane_sum(jnp.where(mine, rate_ref[...], 0.0)) * soft
        matrix = carried_ref[h].reshape(SEQ * DK, DK)
        read = hidot(spread(jnp.concatenate([key, query], axis=0), SEQ), matrix)
        keys = [slab(key, t) for t in range(PROPS)]
        decay = decays([slab(log, t) for t in range(PROPS)])
        done = writes(
            keys,
            [slab(value, t) for t in range(PROPS)],
            [slab(strength, t) for t in range(PROPS)],
            decay,
            [slab(read, t) for t in range(PROPS)],
        )
        for t in range(PROPS):
            q = slab(query, t)
            att = decay[-1, t] * slab(read, PROPS + t)
            for s in range(t + 1):
                weight = lane_sum(keys[s] * q)
                if s < t:
                    weight = decay[s, t] * weight
                att = att + weight * done[s]
            att = att * lax.rsqrt(jnp.mean(att * att, axis=-1, keepdims=True) + epsilon)
            heads_ref[h, pl.ds(t, SEQ, stride=PROPS), :] = att * gain_ref[...] * slab(gate, t)
        head = heads_ref[h].astype(bf16)
        for s in range(ZS):
            out_ref[s, :, lo:hi] = head


def project_kernel(x_ref, heads_ref, w0, w1, w2, w3, out_ref):
    x = x_ref[0]
    rows = heads_ref[...].reshape(GROUP, COLS)
    for r, w in enumerate((w0, w1, w2, w3)):
        at = lax.rem(x + XS - r, XS)
        part = jnp.dot(rows, w[...], preferred_element_type=f32).astype(bf16)
        out_ref[pl.ds(at * TP, TP)] = part.reshape(TP, ROWS, 128)


def final_kernel(terms_ref, out_ref):
    for s in range(XS):
        total = terms_ref[s * TP].astype(f32)
        for t in range(1, TP):
            total = total + terms_ref[s * TP + t].astype(f32)
        out_ref[pl.ds(s * ROWS, ROWS), :] = total.astype(bf16)


def call(kernel, out, specs, flops, scratch=(), grant=16384, placed=None):
    return pl.pallas_call(
        kernel,
        out_shape=out,
        in_specs=specs,
        out_specs=placed or jax.tree.map(lambda _: VMEM, out),
        scratch_shapes=scratch,
        compiler_params=pltpu.CompilerParams(vmem_limit_bytes=grant * 1024),
        cost_estimate=pl.CostEstimate(flops=flops, bytes_accessed=1 << 20, transcendentals=0),
    )


def shift(shard, step, axis="x"):
    return lax.ppermute(shard, axis, ring(step, lax.axis_size(axis)))


def exchange(blocks, axes):
    return lax.all_to_all(blocks, axes, 0, 0, tiled=True)


def step(
    tokens,
    norm_gain,
    w_query,
    w_key,
    w_value,
    w_gate,
    w_decay,
    w_beta,
    decay_rate,
    head_gain,
    w_out,
    state,
    prev_keys,
    prev_values,
    prev_log_decay,
    prev_beta,
    accepted,
):
    z = lax.axis_index("z")
    x = lax.axis_index("x")
    tp = lax.axis_index("tp")
    shape = jax.ShapeDtypeStruct
    zs, xs, tps = (i.astype(jnp.int32).reshape(1) for i in (z, x, tp))

    blocks = call(blocks_kernel, shape((XS, GROUP, 128), bf16), [VMEM], 1 << 20)(
        tokens.reshape(ZS, XS, ROWS, 128)
    )
    tok = exchange(blocks, "x")

    w_qk = jnp.concatenate([w_query, w_key], axis=1)
    w_vz = jnp.concatenate([w_value, w_gate], axis=1)
    qk1 = shift(w_qk, 1)
    vz3 = shift(w_vz, -1)
    vz1 = shift(w_vz, 1)
    qk3 = shift(w_qk, -1)
    qk2 = shift(qk1, 1)
    vz2 = shift(vz3, -1)

    types = [f32 if d in (0, FOLD) else bf16 for d in range(ZS)]
    own, *block = call(
        columns_kernel,
        [shape((ROWS, WIDE), t) for t in types],
        [SMEM] * 3 + [VMEM] * 12,
        2 * GROUP * 512 * 2048,
        [pltpu.VMEM((GROUP, 512), bf16)] * 2,
    )(
        zs, xs, tps, tok, norm_gain.reshape(ZS * XS, 128), w_decay.T, w_beta.T,
        w_qk, qk1, qk2, qk3, w_vz, vz1, vz2, vz3,
    )
    came = {4: shift(block[3], -1, "z")}
    for d in (3, 2, 6, 1, 7):
        came[d] = shift(block[d - 1], d, "z")
    folded = call(fold_kernel, shape((ROWS, WIDE), bf16), [VMEM] * 2, 1 << 20)(came.pop(4), block[4])
    came[5] = shift(folded, 5, "z")

    o1 = shift(w_out, 1)
    o3 = shift(w_out, -1)
    o2 = shift(o1, 1)

    keep = (jnp.arange(PROPS)[None, :] < accepted[:, None]).astype(f32)[:, None, :]
    logs = (prev_log_decay * keep).reshape(SEQ, HEADS * PROPS)
    strengths = (prev_beta * keep).reshape(SEQ, HEADS * PROPS)
    old_keys = prev_keys.astype(f32).transpose(1, 2, 0, 3).reshape(HEADS, ROWS, DK)
    old_values = prev_values.astype(f32).transpose(1, 2, 0, 3).reshape(HEADS, ROWS, DK)
    whole = shape(state.shape, f32)
    buffer = pltpu.VMEM((HEADS, SEQ, DK, DK), f32)
    carried, near = call(
        carried_kernel,
        (whole, shape((HEADS, SEQ, DK, DK), f32)),
        [ANY] + [VMEM] * 4,
        1 << 31,
        [buffer, buffer, pltpu.SemaphoreType.DMA((2, HEADS))],
        16384,
        (ANY, VMEM),
    )(state, old_keys, old_values, logs, strengths)

    heads = call(
        attend_kernel,
        shape((ZS, ROWS, COLS), bf16),
        [SMEM] + [VMEM] * 10,
        1 << 30,
        [
            pltpu.VMEM((1 + 4 * HEADS, ROWS, DK), f32),
            pltpu.VMEM((HEADS, ROWS, DK), f32),
        ],
    )(tps, decay_rate.reshape(1, HEADS * TP), near, head_gain.reshape(1, 128), own, *came.values())
    heads = exchange(heads, "z")
    terms = call(
        project_kernel,
        shape((XS * TP, ROWS, 128), bf16),
        [SMEM] + [VMEM] * 5,
        2 * GROUP * 512 * 512,
    )(xs, heads, w_out, o1, o2, o3)
    terms = exchange(terms, ("x", "tp"))
    mixed = call(final_kernel, shape((XS * ROWS, 128), bf16), [VMEM], 1 << 20)(terms)
    return (mixed.reshape(XS * SEQ, PROPS, 128), carried)


def solution(mesh):
    grid = Mesh(mesh.devices.reshape(ZS, XS, TP), ("z", "x", "tp"))
    kv = ("z", "x")
    placed = (
        P(None, None, kv),
        P(),
        P(kv, "tp"),
        P(kv, "tp"),
        P(kv, "tp"),
        P(kv, "tp"),
        P(),
        P(),
        P(),
        P(),
        P("tp", kv),
        P(kv, "tp", None, None),
        P(kv, "tp", None, None),
        P(kv, "tp", None, None),
        P(kv, "tp", None),
        P(kv, "tp", None),
        P(kv),
    )
    return jax.shard_map(
        step,
        mesh=grid,
        in_specs=placed,
        out_specs=(P("tp", None, kv), P(kv, "tp", None, None)),
        check_vma=False,
    )
```

```python
import jax
import jax.numpy as jnp
from jax import lax
from jax.experimental import pallas as pl
from jax.experimental.pallas import tpu as pltpu
from jax.sharding import Mesh
from jax.sharding import PartitionSpec as P

epsilon = 1e-06
ZS, XS, TP = (8, 4, 8)
PROPS = 4
SEQ = 8
HEADS = 4
DK = 128
ROWS = SEQ * PROPS
GROUP = ZS * ROWS
COLS = HEADS * DK
WIDE = 4 * COLS + 128
FOLD = ZS // 2 + 1
f32 = jnp.float32
bf16 = jnp.bfloat16


VMEM = pl.BlockSpec(memory_space=pltpu.VMEM)
ANY = pl.BlockSpec(memory_space=pl.ANY)
SMEM = pl.BlockSpec(memory_space=pltpu.SMEM)


def ring(step, size):
    return [(i, (i + step) % size) for i in range(size)]


def hidot(a, b):
    return lax.dot_general(
        a, b, (((1,), (0,)), ((), ())), precision=lax.Precision.HIGHEST, preferred_element_type=f32
    )


def spread(rows, matrix_count):
    which = lax.broadcasted_iota(jnp.int32, rows.shape, 0) % matrix_count
    return jnp.concatenate([jnp.where(which == j, rows, 0.0) for j in range(matrix_count)], axis=1)


def lane_sum(a):
    return jnp.sum(a, axis=-1, keepdims=True)


def slab(a, t):
    return a[t * SEQ : (t + 1) * SEQ]


def decays(logs):
    table = {}
    for s in range(-1, PROPS):
        total = None
        for t in range(s + 1, PROPS):
            total = logs[t] if total is None else total + logs[t]
            table[s, t] = jnp.exp(total)
        table[s, s] = None
    return table


def writes(keys, values, strength, decay, read):
    done = []
    for t in range(PROPS):
        predicted = decay[-1, t] * read[t]
        for s in range(t):
            predicted = predicted + (decay[s, t] * lane_sum(keys[s] * keys[t])) * done[s]
        done.append(strength[t] * (values[t] - predicted))
    return done


def head_copies(outer, inner, sems, inward):
    pairs = [(outer.at[:, h], inner.at[h]) for h in range(HEADS)]
    return [
        pltpu.make_async_copy(*(pair if inward else pair[::-1]), sems.at[h]) for h, pair in enumerate(pairs)
    ]


def carried_kernel(
    state_ref, keys_ref, values_ref, logs_ref, beta_ref, taken_ref, out_ref, near_ref, old_ref, new_ref, rows_ref, sems
):
    loads = head_copies(state_ref, old_ref, sems.at[0], True)
    stores = head_copies(out_ref, new_ref, sems.at[1], False)
    for load in loads:
        load.start()
    lane = lax.broadcasted_iota(jnp.int32, (DK, ROWS), 1) % SEQ
    many = HEADS * PROPS

    def to_columns(rows):
        same = lax.broadcasted_iota(jnp.int32, (many, many), 0) == lax.broadcasted_iota(
            jnp.int32, (many, many), 1
        )
        return lax.dot_general(
            rows,
            jnp.where(same, 1.0, 0.0),
            (((0,), (0,)), ((), ())),
            precision=lax.Precision.HIGHEST,
            preferred_element_type=f32,
        )

    taken = to_columns(jnp.broadcast_to(taken_ref[...].astype(f32), (many, SEQ)))
    which = lax.broadcasted_iota(jnp.int32, (SEQ, many), 1) % PROPS
    keep = jnp.where(which.astype(f32) < taken, 1.0, 0.0)
    all_logs = to_columns(logs_ref[...]) * keep
    all_strengths = to_columns(beta_ref[...]) * keep
    rows_ref[0] = keys_ref[...].astype(f32)
    rows_ref[1] = values_ref[...].astype(f32)

    def taken_rows(index, h):
        return jnp.concatenate(
            [rows_ref[index, pl.ds(h * PROPS + t, SEQ, stride=many), :] for t in range(PROPS)], axis=0
        )

    for h in range(HEADS):
        raw = taken_rows(0, h)
        unit = raw * lax.rsqrt(lane_sum(raw * raw) + epsilon)
        vals = taken_rows(1, h)
        loads[h].wait()
        matrix = old_ref[h].reshape(SEQ * DK, DK)
        read = hidot(spread(unit, SEQ), matrix)
        keys = [slab(unit, t) for t in range(PROPS)]
        col = lambda a, t: a[:, h * PROPS + t : h * PROPS + t + 1]
        logs = [col(all_logs, t) for t in range(PROPS)]
        strength = [col(all_strengths, t) for t in range(PROPS)]
        decay = decays(logs)
        done = writes(
            keys, [slab(vals, t) for t in range(PROPS)], strength, decay, [slab(read, t) for t in range(PROPS)]
        )
        last = PROPS - 1
        scaled = [keys[t] if t == last else decay[t, last] * keys[t] for t in range(PROPS)]
        kcols = jnp.concatenate(scaled, axis=0).T
        urows = jnp.concatenate(done, axis=0)
        for j in range(SEQ):
            step = hidot(jnp.where(lane == j, kcols, 0.0), urows)
            keep = decay[-1, last][j : j + 1, :]
            fresh = keep * old_ref[h, j] + step
            new_ref[h, j] = fresh
            near_ref[h, j] = fresh
        stores[h].start()
    for store in stores:
        store.wait()


def blocks_kernel(x_ref, tok_ref, *out_refs):
    for r, ref in enumerate(out_refs):
        at = lax.rem(x_ref[0] + r, XS)
        for d in range(ZS):
            ref[d * ROWS : (d + 1) * ROWS, :] = tok_ref[d, at]


def small_kernel(z_ref, gain_ref, decay_ref, beta_ref, near_gain_ref, near_ref):
    for s in range(XS):
        at = z_ref[0] * XS + s
        lanes = pl.ds(pl.multiple_of(at * 128, 128), 128)
        near_gain_ref[s] = gain_ref[pl.ds(at, 1), :]
        near_ref[s] = jnp.concatenate([decay_ref[:, lanes], beta_ref[:, lanes]], axis=0)


def columns_kernel(z_ref, x_ref, tp_ref, gain_ref, small_ref, *refs):
    toks, pieces, (own_ref, *block_refs, high_ref, low_ref) = (refs[:XS], refs[XS:15], refs[15:])
    z, x, tp = (z_ref[0], x_ref[0], tp_ref[0])
    every = jnp.zeros((GROUP, 2 * HEADS * TP), f32)
    squares = jnp.zeros((GROUP, 128), f32)
    for r in range(XS):
        at = lax.rem(x + XS - r, XS)
        feats = jnp.concatenate(
            [
                toks[r][pl.ds(pl.multiple_of(lax.rem(z + d, ZS) * ROWS, ROWS), ROWS), :]
                for d in range(ZS)
            ],
            axis=0,
        ).astype(f32)
        squares = squares + feats * feats
        feats = feats * gain_ref[at]
        high = feats.astype(bf16)
        low = (feats - high.astype(f32)).astype(bf16)
        high_ref[:, r * 128 : (r + 1) * 128] = high
        low_ref[:, r * 128 : (r + 1) * 128] = low
        small = small_ref[at]
        for part in (high, low):
            every = every + lax.dot_general(
                part, small, (((1,), (1,)), ((), ())), preferred_element_type=f32
            )
    row = lax.broadcasted_iota(jnp.int32, (2 * HEADS * TP, 16), 0)
    col = lax.broadcasted_iota(jnp.int32, (2 * HEADS * TP, 16), 1)
    wanted = jnp.where(col < HEADS, col, col - HEADS + HEADS * TP) + tp * HEADS
    pick = jnp.logical_and(row == wanted, col < 2 * HEADS)
    extra = hidot(every, jnp.where(pick, 1.0, 0.0))
    col = lax.broadcasted_iota(jnp.int32, (GROUP, 16), 1)
    extra = jnp.where(col == 2 * HEADS, lane_sum(squares), extra)
    high = high_ref[...]
    low = low_ref[...]

    def put(lo, hi, part):
        for d in range(ZS):
            rows = part[d * ROWS : (d + 1) * ROWS]
            if d == 0:
                own_ref[:, lo:hi] = rows
            else:
                ref = block_refs[d - 1]
                ref[:, lo:hi] = rows.astype(ref.dtype)

    for pair in range(2):
        for half in range(2):
            cols = slice(half * COLS, (half + 1) * COLS)
            if pair == 0:
                mine = [pieces[0][:, cols]] + [w[...] for w in pieces[1 + 3 * half : 4 + 3 * half]]
            else:
                mine = [w[:, cols] for w in pieces[7:]]
            weight = jnp.concatenate(mine, axis=0)
            at = (2 * pair + half) * COLS
            total = jnp.dot(high, weight, preferred_element_type=f32)
            total = total + jnp.dot(low, weight, preferred_element_type=f32)
            put(at, at + COLS, total)
    zero = jnp.zeros((GROUP, 112), f32)
    put(4 * COLS, WIDE, jnp.concatenate([extra, zero], axis=1))
    rest = extra - extra.astype(bf16).astype(f32)
    for d in range(1, ZS):
        if d != FOLD:
            rows = rest[d * ROWS : (d + 1) * ROWS]
            block_refs[d - 1][:, 4 * COLS + 16 : 4 * COLS + 32] = rows.astype(bf16)


def fold_kernel(came_ref, own_ref, out_ref):
    total = came_ref[...].astype(f32) + own_ref[...]
    out_ref[...] = total.astype(bf16)
    at = 4 * COLS
    extra = total[:, at : at + 16] + total[:, at + 16 : at + 32]
    high = extra.astype(bf16)
    out_ref[:, at : at + 16] = high
    out_ref[:, at + 16 : at + 32] = (extra - high.astype(f32)).astype(bf16)


def unit(a):
    return a * lax.rsqrt(lane_sum(a * a) + epsilon)


def silu(a):
    return a * jax.nn.sigmoid(a)


def attend_kernel(tp_ref, rate_ref, carried_ref, gain_ref, own_ref, *refs):
    came, (out_ref, rows_ref, heads_ref) = (refs[:-3], refs[-3:])

    def total(lo, hi):
        acc = own_ref[:, lo:hi]
        for ref in came:
            acc = acc + ref[:, lo:hi].astype(f32)
        return acc

    def regroup(index, rows):
        rows_ref[index] = rows
        return jnp.concatenate(
            [rows_ref[index, pl.ds(t, SEQ, stride=PROPS), :] for t in range(PROPS)], axis=0
        )

    extra = regroup(0, total(4 * COLS, WIDE))
    extra = extra[:, :16] + extra[:, 16:32]
    scale = lax.rsqrt(extra[:, 2 * HEADS : 2 * HEADS + 1] / 4096 + epsilon)

    def raw(index, lo, hi):
        return regroup(index, total(lo, hi)) * scale

    for h in range(HEADS):
        lo, hi = (h * DK, (h + 1) * DK)
        spot = 1 + 4 * h
        query = unit(silu(raw(spot, lo, hi))) * DK ** (-0.5)
        key = unit(silu(raw(spot + 1, COLS + lo, COLS + hi)))
        value = silu(raw(spot + 2, 2 * COLS + lo, 2 * COLS + hi))
        gate = silu(raw(spot + 3, 3 * COLS + lo, 3 * COLS + hi))
        araw = extra[:, h : h + 1] * scale
        braw = extra[:, HEADS + h : HEADS + h + 1] * scale
        strength = jax.nn.sigmoid(braw)
        soft = jnp.maximum(araw, 0.0) + jnp.log1p(jnp.exp(-jnp.abs(araw)))
        mine = lax.broadcasted_iota(jnp.int32, rate_ref.shape, 1) == tp_ref[0] * HEADS + h
        log = -lane_sum(jnp.where(mine, rate_ref[...], 0.0)) * soft
        matrix = carried_ref[h].reshape(SEQ * DK, DK)
        read = hidot(spread(jnp.concatenate([key, query], axis=0), SEQ), matrix)
        keys = [slab(key, t) for t in range(PROPS)]
        decay = decays([slab(log, t) for t in range(PROPS)])
        done = writes(
            keys,
            [slab(value, t) for t in range(PROPS)],
            [slab(strength, t) for t in range(PROPS)],
            decay,
            [slab(read, t) for t in range(PROPS)],
        )
        for t in range(PROPS):
            q = slab(query, t)
            att = decay[-1, t] * slab(read, PROPS + t)
            for s in range(t + 1):
                weight = lane_sum(keys[s] * q)
                if s < t:
                    weight = decay[s, t] * weight
                att = att + weight * done[s]
            att = att * lax.rsqrt(jnp.mean(att * att, axis=-1, keepdims=True) + epsilon)
            heads_ref[h, pl.ds(t, SEQ, stride=PROPS), :] = att * gain_ref[...] * slab(gate, t)
        head = heads_ref[h].astype(bf16)
        for s in range(ZS):
            out_ref[s, :, lo:hi] = head


def project_kernel(x_ref, heads_ref, w0, w1, w2, w3, out_ref):
    x = x_ref[0]
    rows = heads_ref[...].reshape(GROUP, COLS)
    for r, w in enumerate((w0, w1, w2, w3)):
        at = lax.rem(x + XS - r, XS)
        part = jnp.dot(rows, w[...], preferred_element_type=f32).astype(bf16)
        out_ref[pl.ds(at * TP, TP)] = part.reshape(TP, ROWS, 128)


def final_kernel(terms_ref, out_ref):
    for s in range(XS):
        total = terms_ref[s * TP].astype(f32)
        for t in range(1, TP):
            total = total + terms_ref[s * TP + t].astype(f32)
        out_ref[pl.ds(s * ROWS, ROWS), :] = total.astype(bf16)


def call(kernel, out, specs, flops, scratch=(), grant=16384, placed=None):
    return pl.pallas_call(
        kernel,
        out_shape=out,
        in_specs=specs,
        out_specs=placed or jax.tree.map(lambda _: VMEM, out),
        scratch_shapes=scratch,
        compiler_params=pltpu.CompilerParams(vmem_limit_bytes=grant * 1024),
        cost_estimate=pl.CostEstimate(flops=flops, bytes_accessed=1 << 20, transcendentals=0),
    )


def shift(shard, step, axis="x"):
    return lax.ppermute(shard, axis, ring(step, lax.axis_size(axis)))


def exchange(blocks, axes):
    return lax.all_to_all(blocks, axes, 0, 0, tiled=True)


def step(
    tokens,
    norm_gain,
    w_query,
    w_key,
    w_value,
    w_gate,
    w_decay,
    w_beta,
    decay_rate,
    head_gain,
    w_out,
    state,
    prev_keys,
    prev_values,
    prev_log_decay,
    prev_beta,
    accepted,
):
    z = lax.axis_index("z")
    x = lax.axis_index("x")
    tp = lax.axis_index("tp")
    shape = jax.ShapeDtypeStruct
    zs, xs, tps = (i.astype(jnp.int32).reshape(1) for i in (z, x, tp))

    t0, *away = call(
        blocks_kernel, [shape((GROUP, 128), bf16)] * XS, [SMEM, VMEM], 1 << 20
    )(xs, tokens.reshape(ZS, XS, ROWS, 128))
    t1, t2, t3 = (shift(away[r - 1], r) for r in range(1, XS))

    q1 = shift(w_query, 1)
    q3 = shift(w_query, -1)
    k1 = shift(w_key, 1)
    k3 = shift(w_key, -1)
    w_vz = jnp.concatenate([w_value, w_gate], axis=1)
    vz3 = shift(w_vz, -1)
    vz1 = shift(w_vz, 1)
    q2 = shift(q1, 1)
    k2 = shift(k1, 1)
    vz2 = shift(vz3, -1)
    w_qk = jnp.concatenate([w_query, w_key], axis=1)

    gain, small = call(
        small_kernel,
        (shape((XS, 1, 128), f32), shape((XS, 2 * HEADS * TP, 128), bf16)),
        [SMEM] + [VMEM] * 3,
        1 << 10,
    )(zs, norm_gain.reshape(ZS * XS, 128), w_decay.T, w_beta.T)

    types = [f32 if d in (0, FOLD) else bf16 for d in range(ZS)]
    own, *block = call(
        columns_kernel,
        [shape((ROWS, WIDE), t) for t in types],
        [SMEM] * 3 + [VMEM] * 17,
        2 * GROUP * 512 * 2048,
        [pltpu.VMEM((GROUP, 512), bf16)] * 2,
    )(
        zs, xs, tps, gain, small, t0, t1, t2, t3,
        w_qk, q1, q2, q3, k1, k2, k3, w_vz, vz1, vz2, vz3,
    )
    came = {4: shift(block[3], -1, "z")}
    for d in (3, 2, 6, 1, 7):
        came[d] = shift(block[d - 1], d, "z")
    folded = call(fold_kernel, shape((ROWS, WIDE), bf16), [VMEM] * 2, 1 << 20)(came.pop(4), block[4])
    came[5] = shift(folded, 5, "z")

    o1 = shift(w_out, 1)
    o3 = shift(w_out, -1)
    o2 = shift(o1, 1)

    whole = shape(state.shape, f32)
    flat = (SEQ * HEADS * PROPS, DK)
    by_sequence = lambda a: a.transpose(1, 2, 0).reshape(HEADS * PROPS, SEQ)
    buffer = pltpu.VMEM((HEADS, SEQ, DK, DK), f32)
    carried, near = call(
        carried_kernel,
        (whole, shape((HEADS, SEQ, DK, DK), f32)),
        [ANY] + [VMEM] * 5,
        1 << 31,
        [buffer, buffer, pltpu.VMEM((2, *flat), f32), pltpu.SemaphoreType.DMA((2, HEADS))],
        16384,
        (ANY, VMEM),
    )(
        state,
        prev_keys.reshape(flat),
        prev_values.reshape(flat),
        by_sequence(prev_log_decay),
        by_sequence(prev_beta),
        accepted.reshape(1, SEQ),
    )

    heads = call(
        attend_kernel,
        shape((ZS, ROWS, COLS), bf16),
        [SMEM] + [VMEM] * 10,
        1 << 30,
        [
            pltpu.VMEM((1 + 4 * HEADS, ROWS, DK), f32),
            pltpu.VMEM((HEADS, ROWS, DK), f32),
        ],
    )(tps, decay_rate.reshape(1, HEADS * TP), near, head_gain.reshape(1, 128), own, *came.values())
    heads = exchange(heads, "z")
    terms = call(
        project_kernel,
        shape((XS * TP, ROWS, 128), bf16),
        [SMEM] + [VMEM] * 5,
        2 * GROUP * 512 * 512,
    )(xs, heads, w_out, o1, o2, o3)
    terms = exchange(terms, ("x", "tp"))
    mixed = call(final_kernel, shape((XS * ROWS, 128), bf16), [VMEM], 1 << 20)(terms)
    return (mixed.reshape(XS * SEQ, PROPS, 128), carried)


def solution(mesh):
    grid = Mesh(mesh.devices.reshape(ZS, XS, TP), ("z", "x", "tp"))
    kv = ("z", "x")
    placed = (
        P(None, None, kv),
        P(),
        P(kv, "tp"),
        P(kv, "tp"),
        P(kv, "tp"),
        P(kv, "tp"),
        P(),
        P(),
        P(),
        P(),
        P("tp", kv),
        P(kv, "tp", None, None),
        P(kv, "tp", None, None),
        P(kv, "tp", None, None),
        P(kv, "tp", None),
        P(kv, "tp", None),
        P(kv),
    )
    return jax.shard_map(
        step,
        mesh=grid,
        in_specs=placed,
        out_specs=(P("tp", None, kv), P(kv, "tp", None, None)),
        check_vma=False,
    )
```

```python
import jax
import jax.numpy as jnp
from jax import lax
from jax.experimental import pallas as pl
from jax.experimental.pallas import tpu as pltpu
from jax.sharding import Mesh
from jax.sharding import PartitionSpec as P

epsilon = 1e-06
ZS, XS, TP = (8, 4, 8)
PROPS = 4
SEQ = 8
HEADS = 4
DK = 128
ROWS = SEQ * PROPS
GROUP = ZS * ROWS
COLS = HEADS * DK
WIDE = 4 * COLS + 128
FOLD = ZS // 2 + 1
f32 = jnp.float32
bf16 = jnp.bfloat16


VMEM = pl.BlockSpec(memory_space=pltpu.VMEM)
ANY = pl.BlockSpec(memory_space=pl.ANY)
SMEM = pl.BlockSpec(memory_space=pltpu.SMEM)


def ring(step, size):
    return [(i, (i + step) % size) for i in range(size)]


def hidot(a, b):
    return lax.dot_general(
        a, b, (((1,), (0,)), ((), ())), precision=lax.Precision.HIGHEST, preferred_element_type=f32
    )


def halves(a):
    high = a.astype(bf16)
    return high, (a - high.astype(f32)).astype(bf16)


def neardot(a, b):
    (ah, al), (bh, bl) = (halves(a), halves(b))
    dot = lambda u, v: jnp.dot(u, v, preferred_element_type=f32)
    return dot(ah, bh) + dot(ah, bl) + dot(al, bh)


def spread(rows, matrix_count):
    which = lax.broadcasted_iota(jnp.int32, rows.shape, 0) % matrix_count
    return jnp.concatenate([jnp.where(which == j, rows, 0.0) for j in range(matrix_count)], axis=1)


def lane_sum(a):
    return jnp.sum(a, axis=-1, keepdims=True)


def slab(a, t):
    return a[t * SEQ : (t + 1) * SEQ]


def decays(logs):
    table = {}
    for s in range(-1, PROPS):
        total = None
        for t in range(s + 1, PROPS):
            total = logs[t] if total is None else total + logs[t]
            table[s, t] = jnp.exp(total)
        table[s, s] = None
    return table


def writes(keys, values, strength, decay, read):
    done = []
    for t in range(PROPS):
        predicted = decay[-1, t] * read[t]
        for s in range(t):
            predicted = predicted + (decay[s, t] * lane_sum(keys[s] * keys[t])) * done[s]
        done.append(strength[t] * (values[t] - predicted))
    return done


def head_copies(outer, inner, sems, inward):
    pairs = [(outer.at[:, h], inner.at[h]) for h in range(HEADS)]
    return [
        pltpu.make_async_copy(*(pair if inward else pair[::-1]), sems.at[h]) for h, pair in enumerate(pairs)
    ]


def carried_kernel(
    state_ref, keys_ref, values_ref, logs_ref, beta_ref, taken_ref, out_ref, near_ref, old_ref, new_ref, rows_ref, sems
):
    loads = head_copies(state_ref, old_ref, sems.at[0], True)
    stores = head_copies(out_ref, new_ref, sems.at[1], False)
    for load in loads:
        load.start()
    lane = lax.broadcasted_iota(jnp.int32, (DK, ROWS), 1) % SEQ
    many = HEADS * PROPS

    def to_columns(rows):
        same = lax.broadcasted_iota(jnp.int32, (many, many), 0) == lax.broadcasted_iota(
            jnp.int32, (many, many), 1
        )
        return lax.dot_general(
            rows,
            jnp.where(same, 1.0, 0.0),
            (((0,), (0,)), ((), ())),
            precision=lax.Precision.HIGHEST,
            preferred_element_type=f32,
        )

    taken = to_columns(jnp.broadcast_to(taken_ref[...].astype(f32), (many, SEQ)))
    which = lax.broadcasted_iota(jnp.int32, (SEQ, many), 1) % PROPS
    keep = jnp.where(which.astype(f32) < taken, 1.0, 0.0)
    all_logs = to_columns(logs_ref[...]) * keep
    all_strengths = to_columns(beta_ref[...]) * keep
    rows_ref[0] = keys_ref[...].astype(f32)
    rows_ref[1] = values_ref[...].astype(f32)

    def taken_rows(index, h):
        return jnp.concatenate(
            [rows_ref[index, pl.ds(h * PROPS + t, SEQ, stride=many), :] for t in range(PROPS)], axis=0
        )

    for h in range(HEADS):
        raw = taken_rows(0, h)
        unit = raw * lax.rsqrt(lane_sum(raw * raw) + epsilon)
        vals = taken_rows(1, h)
        loads[h].wait()
        matrix = old_ref[h].reshape(SEQ * DK, DK)
        read = neardot(spread(unit, SEQ), matrix)
        keys = [slab(unit, t) for t in range(PROPS)]
        col = lambda a, t: a[:, h * PROPS + t : h * PROPS + t + 1]
        logs = [col(all_logs, t) for t in range(PROPS)]
        strength = [col(all_strengths, t) for t in range(PROPS)]
        decay = decays(logs)
        done = writes(
            keys, [slab(vals, t) for t in range(PROPS)], strength, decay, [slab(read, t) for t in range(PROPS)]
        )
        last = PROPS - 1
        scaled = [keys[t] if t == last else decay[t, last] * keys[t] for t in range(PROPS)]
        kcols = jnp.concatenate(scaled, axis=0).T
        urows = jnp.concatenate(done, axis=0)
        step = neardot(jnp.concatenate([jnp.where(lane == j, kcols, 0.0) for j in range(SEQ)], axis=0), urows)
        for j in range(SEQ):
            keep = decay[-1, last][j : j + 1, :]
            fresh = keep * old_ref[h, j] + step[j * DK : (j + 1) * DK]
            new_ref[h, j] = fresh
            near_ref[h, j] = fresh
        stores[h].start()
    for store in stores:
        store.wait()


def blocks_kernel(x_ref, tok_ref, *out_refs):
    for r, ref in enumerate(out_refs):
        at = lax.rem(x_ref[0] + r, XS)
        for d in range(ZS):
            ref[d * ROWS : (d + 1) * ROWS, :] = tok_ref[d, at]


def small_kernel(z_ref, gain_ref, decay_ref, beta_ref, near_gain_ref, near_ref):
    for s in range(XS):
        at = z_ref[0] * XS + s
        lanes = pl.ds(pl.multiple_of(at * 128, 128), 128)
        near_gain_ref[s] = gain_ref[pl.ds(at, 1), :]
        near_ref[s] = jnp.concatenate([decay_ref[:, lanes], beta_ref[:, lanes]], axis=0)


def columns_kernel(z_ref, x_ref, tp_ref, gain_ref, small_ref, *refs):
    toks, pieces, (own_ref, *block_refs, high_ref, low_ref) = (refs[:XS], refs[XS:15], refs[15:])
    z, x, tp = (z_ref[0], x_ref[0], tp_ref[0])
    every = jnp.zeros((GROUP, 2 * HEADS * TP), f32)
    squares = jnp.zeros((GROUP, 128), f32)
    for r in range(XS):
        at = lax.rem(x + XS - r, XS)
        feats = jnp.concatenate(
            [
                toks[r][pl.ds(pl.multiple_of(lax.rem(z + d, ZS) * ROWS, ROWS), ROWS), :]
                for d in range(ZS)
            ],
            axis=0,
        ).astype(f32)
        squares = squares + feats * feats
        feats = feats * gain_ref[at]
        high = feats.astype(bf16)
        low = (feats - high.astype(f32)).astype(bf16)
        high_ref[:, r * 128 : (r + 1) * 128] = high
        low_ref[:, r * 128 : (r + 1) * 128] = low
        small = small_ref[at]
        for part in (high, low):
            every = every + lax.dot_general(
                part, small, (((1,), (1,)), ((), ())), preferred_element_type=f32
            )
    row = lax.broadcasted_iota(jnp.int32, (2 * HEADS * TP, 16), 0)
    col = lax.broadcasted_iota(jnp.int32, (2 * HEADS * TP, 16), 1)
    wanted = jnp.where(col < HEADS, col, col - HEADS + HEADS * TP) + tp * HEADS
    pick = jnp.logical_and(row == wanted, col < 2 * HEADS)
    extra = hidot(every, jnp.where(pick, 1.0, 0.0))
    col = lax.broadcasted_iota(jnp.int32, (GROUP, 16), 1)
    extra = jnp.where(col == 2 * HEADS, lane_sum(squares), extra)
    high = high_ref[...]
    low = low_ref[...]

    def put(lo, hi, part):
        for d in range(ZS):
            rows = part[d * ROWS : (d + 1) * ROWS]
            if d == 0:
                own_ref[:, lo:hi] = rows
            else:
                ref = block_refs[d - 1]
                ref[:, lo:hi] = rows.astype(ref.dtype)

    for pair in range(2):
        for half in range(2):
            cols = slice(half * COLS, (half + 1) * COLS)
            if pair == 0:
                mine = [pieces[0][:, cols]] + [w[...] for w in pieces[1 + 3 * half : 4 + 3 * half]]
            else:
                mine = [w[:, cols] for w in pieces[7:]]
            weight = jnp.concatenate(mine, axis=0)
            at = (2 * pair + half) * COLS
            total = jnp.dot(high, weight, preferred_element_type=f32)
            total = total + jnp.dot(low, weight, preferred_element_type=f32)
            put(at, at + COLS, total)
    zero = jnp.zeros((GROUP, 112), f32)
    put(4 * COLS, WIDE, jnp.concatenate([extra, zero], axis=1))
    rest = extra - extra.astype(bf16).astype(f32)
    for d in range(1, ZS):
        if d != FOLD:
            rows = rest[d * ROWS : (d + 1) * ROWS]
            block_refs[d - 1][:, 4 * COLS + 16 : 4 * COLS + 32] = rows.astype(bf16)


def fold_kernel(came_ref, own_ref, out_ref):
    total = came_ref[...].astype(f32) + own_ref[...]
    out_ref[...] = total.astype(bf16)
    at = 4 * COLS
    extra = total[:, at : at + 16] + total[:, at + 16 : at + 32]
    high = extra.astype(bf16)
    out_ref[:, at : at + 16] = high
    out_ref[:, at + 16 : at + 32] = (extra - high.astype(f32)).astype(bf16)


def unit(a):
    return a * lax.rsqrt(lane_sum(a * a) + epsilon)


def silu(a):
    return a * jax.nn.sigmoid(a)


def attend_kernel(tp_ref, rate_ref, carried_ref, gain_ref, own_ref, *refs):
    came, (out_ref, rows_ref, heads_ref) = (refs[:-3], refs[-3:])

    def total(lo, hi):
        acc = own_ref[:, lo:hi]
        for ref in came:
            acc = acc + ref[:, lo:hi].astype(f32)
        return acc

    def regroup(index, rows):
        rows_ref[index] = rows
        return jnp.concatenate(
            [rows_ref[index, pl.ds(t, SEQ, stride=PROPS), :] for t in range(PROPS)], axis=0
        )

    extra = regroup(0, total(4 * COLS, WIDE))
    extra = extra[:, :16] + extra[:, 16:32]
    scale = lax.rsqrt(extra[:, 2 * HEADS : 2 * HEADS + 1] / 4096 + epsilon)

    def raw(index, lo, hi):
        return regroup(index, total(lo, hi)) * scale

    for h in range(HEADS):
        lo, hi = (h * DK, (h + 1) * DK)
        spot = 1 + 4 * h
        query = unit(silu(raw(spot, lo, hi))) * DK ** (-0.5)
        key = unit(silu(raw(spot + 1, COLS + lo, COLS + hi)))
        value = silu(raw(spot + 2, 2 * COLS + lo, 2 * COLS + hi))
        gate = silu(raw(spot + 3, 3 * COLS + lo, 3 * COLS + hi))
        araw = extra[:, h : h + 1] * scale
        braw = extra[:, HEADS + h : HEADS + h + 1] * scale
        strength = jax.nn.sigmoid(braw)
        soft = jnp.maximum(araw, 0.0) + jnp.log1p(jnp.exp(-jnp.abs(araw)))
        mine = lax.broadcasted_iota(jnp.int32, rate_ref.shape, 1) == tp_ref[0] * HEADS + h
        log = -lane_sum(jnp.where(mine, rate_ref[...], 0.0)) * soft
        matrix = carried_ref[h].reshape(SEQ * DK, DK)
        read = neardot(spread(jnp.concatenate([key, query], axis=0), SEQ), matrix)
        keys = [slab(key, t) for t in range(PROPS)]
        decay = decays([slab(log, t) for t in range(PROPS)])
        done = writes(
            keys,
            [slab(value, t) for t in range(PROPS)],
            [slab(strength, t) for t in range(PROPS)],
            decay,
            [slab(read, t) for t in range(PROPS)],
        )
        for t in range(PROPS):
            q = slab(query, t)
            att = decay[-1, t] * slab(read, PROPS + t)
            for s in range(t + 1):
                weight = lane_sum(keys[s] * q)
                if s < t:
                    weight = decay[s, t] * weight
                att = att + weight * done[s]
            att = att * lax.rsqrt(jnp.mean(att * att, axis=-1, keepdims=True) + epsilon)
            heads_ref[h, pl.ds(t, SEQ, stride=PROPS), :] = att * gain_ref[...] * slab(gate, t)
        head = heads_ref[h].astype(bf16)
        for s in range(ZS):
            out_ref[s, :, lo:hi] = head


def project_kernel(x_ref, heads_ref, w0, w1, w2, w3, out_ref):
    x = x_ref[0]
    rows = heads_ref[...].reshape(GROUP, COLS)
    for r, w in enumerate((w0, w1, w2, w3)):
        at = lax.rem(x + XS - r, XS)
        part = jnp.dot(rows, w[...], preferred_element_type=f32).astype(bf16)
        out_ref[pl.ds(at * TP, TP)] = part.reshape(TP, ROWS, 128)


def final_kernel(terms_ref, out_ref):
    for s in range(XS):
        total = terms_ref[s * TP].astype(f32)
        for t in range(1, TP):
            total = total + terms_ref[s * TP + t].astype(f32)
        out_ref[pl.ds(s * ROWS, ROWS), :] = total.astype(bf16)


def call(kernel, out, specs, flops, scratch=(), grant=16384, placed=None):
    return pl.pallas_call(
        kernel,
        out_shape=out,
        in_specs=specs,
        out_specs=placed or jax.tree.map(lambda _: VMEM, out),
        scratch_shapes=scratch,
        compiler_params=pltpu.CompilerParams(vmem_limit_bytes=grant * 1024),
        cost_estimate=pl.CostEstimate(flops=flops, bytes_accessed=1 << 20, transcendentals=0),
    )


def shift(shard, step, axis="x"):
    return lax.ppermute(shard, axis, ring(step, lax.axis_size(axis)))


def exchange(blocks, axes):
    return lax.all_to_all(blocks, axes, 0, 0, tiled=True)


def step(
    tokens,
    norm_gain,
    w_query,
    w_key,
    w_value,
    w_gate,
    w_decay,
    w_beta,
    decay_rate,
    head_gain,
    w_out,
    state,
    prev_keys,
    prev_values,
    prev_log_decay,
    prev_beta,
    accepted,
):
    z = lax.axis_index("z")
    x = lax.axis_index("x")
    tp = lax.axis_index("tp")
    shape = jax.ShapeDtypeStruct
    zs, xs, tps = (i.astype(jnp.int32).reshape(1) for i in (z, x, tp))

    t0, *away = call(
        blocks_kernel, [shape((GROUP, 128), bf16)] * XS, [SMEM, VMEM], 1 << 20
    )(xs, tokens.reshape(ZS, XS, ROWS, 128))
    t1, t2, t3 = (shift(away[r - 1], r) for r in range(1, XS))

    q1 = shift(w_query, 1)
    q3 = shift(w_query, -1)
    k1 = shift(w_key, 1)
    k3 = shift(w_key, -1)
    w_vz = jnp.concatenate([w_value, w_gate], axis=1)
    vz3 = shift(w_vz, -1)
    vz1 = shift(w_vz, 1)
    q2 = shift(q1, 1)
    k2 = shift(k1, 1)
    vz2 = shift(vz3, -1)
    w_qk = jnp.concatenate([w_query, w_key], axis=1)

    gain, small = call(
        small_kernel,
        (shape((XS, 1, 128), f32), shape((XS, 2 * HEADS * TP, 128), bf16)),
        [SMEM] + [VMEM] * 3,
        1 << 10,
    )(zs, norm_gain.reshape(ZS * XS, 128), w_decay.T, w_beta.T)

    types = [f32 if d in (0, FOLD) else bf16 for d in range(ZS)]
    own, *block = call(
        columns_kernel,
        [shape((ROWS, WIDE), t) for t in types],
        [SMEM] * 3 + [VMEM] * 17,
        2 * GROUP * 512 * 2048,
        [pltpu.VMEM((GROUP, 512), bf16)] * 2,
    )(
        zs, xs, tps, gain, small, t0, t1, t2, t3,
        w_qk, q1, q2, q3, k1, k2, k3, w_vz, vz1, vz2, vz3,
    )
    came = {4: shift(block[3], -1, "z")}
    for d in (3, 2, 6, 1, 7):
        came[d] = shift(block[d - 1], d, "z")
    folded = call(fold_kernel, shape((ROWS, WIDE), bf16), [VMEM] * 2, 1 << 20)(came.pop(4), block[4])
    came[5] = shift(folded, 5, "z")

    o1 = shift(w_out, 1)
    o3 = shift(w_out, -1)
    o2 = shift(o1, 1)

    whole = shape(state.shape, f32)
    flat = (SEQ * HEADS * PROPS, DK)
    by_sequence = lambda a: a.transpose(1, 2, 0).reshape(HEADS * PROPS, SEQ)
    buffer = pltpu.VMEM((HEADS, SEQ, DK, DK), f32)
    carried, near = call(
        carried_kernel,
        (whole, shape((HEADS, SEQ, DK, DK), f32)),
        [ANY] + [VMEM] * 5,
        1 << 31,
        [buffer, buffer, pltpu.VMEM((2, *flat), f32), pltpu.SemaphoreType.DMA((2, HEADS))],
        16384,
        (ANY, VMEM),
    )(
        state,
        prev_keys.reshape(flat),
        prev_values.reshape(flat),
        by_sequence(prev_log_decay),
        by_sequence(prev_beta),
        accepted.reshape(1, SEQ),
    )

    heads = call(
        attend_kernel,
        shape((ZS, ROWS, COLS), bf16),
        [SMEM] + [VMEM] * 10,
        1 << 30,
        [
            pltpu.VMEM((1 + 4 * HEADS, ROWS, DK), f32),
            pltpu.VMEM((HEADS, ROWS, DK), f32),
        ],
    )(tps, decay_rate.reshape(1, HEADS * TP), near, head_gain.reshape(1, 128), own, *came.values())
    heads = exchange(heads, "z")
    terms = call(
        project_kernel,
        shape((XS * TP, ROWS, 128), bf16),
        [SMEM] + [VMEM] * 5,
        2 * GROUP * 512 * 512,
    )(xs, heads, w_out, o1, o2, o3)
    terms = exchange(terms, ("x", "tp"))
    mixed = call(final_kernel, shape((XS * ROWS, 128), bf16), [VMEM], 1 << 20)(terms)
    return (mixed.reshape(XS * SEQ, PROPS, 128), carried)


def solution(mesh):
    grid = Mesh(mesh.devices.reshape(ZS, XS, TP), ("z", "x", "tp"))
    kv = ("z", "x")
    placed = (
        P(None, None, kv),
        P(),
        P(kv, "tp"),
        P(kv, "tp"),
        P(kv, "tp"),
        P(kv, "tp"),
        P(),
        P(),
        P(),
        P(),
        P("tp", kv),
        P(kv, "tp", None, None),
        P(kv, "tp", None, None),
        P(kv, "tp", None, None),
        P(kv, "tp", None),
        P(kv, "tp", None),
        P(kv),
    )
    return jax.shard_map(
        step,
        mesh=grid,
        in_specs=placed,
        out_specs=(P("tp", None, kv), P(kv, "tp", None, None)),
        check_vma=False,
    )
```
